32 devices in a mesh: sp: 4 (over y, x), tp: 8 (over z, core).
Axes of the slice: x: 2, y: 2, z: 4, core: 2. Of those that a mesh axis runs over, the one named last changes fastest.
Arguments:
- skip_stream_entry: bfloat16 [2048, 2048], P(('sp', 'tp')), may hold values from -6 to 6
- result_switch_mapped: bfloat16 [2048, 4096], P('sp', 'tp'), may hold values from -6 to 6
- channel_feed_mapped: bfloat16 [2048, 4096], P('sp', 'tp'), may hold values from -6 to 6
- write_coefficient_mapped: bfloat16 [2048, 2048], P('sp', 'tp'), may hold values from -6 to 6
- emission_coefficient_mapped: bfloat16 [2048, 2048], P('sp', 'tp'), may hold values from -6 to 6
- channel_feed_taps: bfloat16 [5, 4096], P(None, 'tp'), may hold values from -2.5 to 2.5
- write_coefficient_taps: bfloat16 [5, 2048], P(None, 'tp'), may hold values from -2.5 to 2.5
- emission_coefficient_taps: bfloat16 [5, 2048], P(None, 'tp'), may hold values from -2.5 to 2.5
- raw_increments: bfloat16 [2, 64, 2048], P(None, 'tp', 'sp'), may hold values from -6 to 6
- channel_log_fade_speed: float32 [2, 64], P(None, 'tp'), may hold values from -20 to 0
- extra_log_fade: float32 [2, 64, 2048], P(None, 'tp', 'sp'), may hold values from -1 to 0
- cluster_scaling_factor: float32 [4096], P('tp'), may hold values from 0.1 to 1.9
- blend_result_matrix: bfloat16 [4096, 2048], P('tp'), may hold values from -0.09375 to 0.09375
- routing_scaling_factor: float32 [2048], replicated, may hold values from 0.1 to 1.9
- specialist_switch_matrix: bfloat16 [8, 2048, 4096], P('sp', None, 'tp'), may hold values from -0.125 to 0.125
- specialist_widen_matrix: bfloat16 [8, 2048, 4096], P('sp', None, 'tp'), may hold values from -0.125 to 0.125
- specialist_contract_matrix: bfloat16 [8, 4096, 2048], P('sp', 'tp'), may hold values from -0.1875 to 0.1875
- picked_specialists: int32 [2048, 2], P(('sp', 'tp')), may hold values from 0 to 7, all different within a row; in each aligned block of 64 rows (0 to 63, 64 to 127, ...) at most 24 rows name the same one
- router_affinities: float32 [2048, 2], P(('sp', 'tp')), may hold values from 0.1 to 1
Outputs:
- result: bfloat16 [2048, 2048], P(('sp', 'tp'))
The draws below stay inside these ranges and needn't reach their ends.
Inputs may be any that keep to these rules, and one draw needn't show every extreme that they name: `picked_specialists`: each row names 2 different experts. Within the rows of one device (aligned blocks of 64 rows) no expert is named more than 24 times, a bound that some block reaches.
All inputs are finite; a program needn't handle non-finite values.
Results may differ from the reference program's by a relative error of at most 0.02.
Values may be sent and summed in bfloat16 or wider, within the bound.
A program may use at most 64 MiB of HBM per device.

```python
import math
import jax
import jax.numpy as jnp
import numpy as np
from jax import lax

WIDTH = 2048
HEADS = 64
HEAD_DIM = 64
GROUPS = 16
STATE = 128
EXPERT_FF = 4096
CONV_W = 5
BLOCK = 128
TOP = 2
SEQ_DEV = 512
INNER = 4096
SERIES_ITEMS = 2048
ROWS_DEV = 64
EXPERTS = 8
CAPACITY = 24
N_SP = 4
N_TP = 8


def draw_raw_increments(key, part):
    first_key, second_key = jax.random.split(key)
    noise = 0.7 * jax.random.normal(second_key, (2, HEADS, SERIES_ITEMS), jnp.float32)
    shifts = jax.random.uniform(first_key, (2, HEADS, SERIES_ITEMS // SEQ_DEV), jnp.float32, -1.5, 1.0)
    return (noise + jnp.repeat(shifts, SEQ_DEV, axis=2)).astype(jnp.bfloat16)


def draw_channel_log_fade_speed(key, part):
    coin_key, slow_key, fast_key = jax.random.split(key, 3)
    share = 0.5
    slow = jnp.log(jax.random.uniform(slow_key, (2, HEADS), jnp.float32, 0.1, 0.4) / SERIES_ITEMS)
    fast = jnp.log(jax.random.uniform(fast_key, (2, HEADS), jnp.float32, 0.05, 0.12))
    return jnp.where(jax.random.uniform(coin_key, (2, HEADS), jnp.float32) < share, slow, fast)


def draw_extra_log_fade(key, part):
    place_key, depth_key = jax.random.split(key)
    third = SERIES_ITEMS // 3
    offsets = jnp.arange(3, dtype=jnp.int32) * third
    places = offsets[None, None, :] + jax.random.randint(place_key, (2, HEADS, 3), 0, third, dtype=jnp.int32)
    depths = jnp.log(jax.random.uniform(depth_key, (2, HEADS, 3), jnp.float32, 0.5, 0.8))
    positions = jnp.arange(SERIES_ITEMS, dtype=jnp.int32)
    landed = positions[None, None, None, :] == places[..., None]
    return jnp.sum(jnp.where(landed, depths[..., None], 0.0), axis=2)


def level_of(rng, dims, cuts, least, largest):
    level, own = 1.0, jax.random.fold_in(rng, 6)
    for position, blocks in cuts:
        heights = jnp.exp(jax.random.uniform(jax.random.fold_in(own, position), (blocks,), jnp.float32, least / len(cuts), largest / len(cuts)))
        level = level * jnp.repeat(heights, dims[position] // blocks).reshape([-1 if axis == position else 1 for axis in range(len(dims))])
    return level


def shared_out(stream_key, own, number, rows, number_of, top, bound, skew):
    order = jax.random.permutation(stream_key, number_of)
    heavy_load, common = load_shares(number_of, rows * top, bound, skew, True), load_shares(number_of, rows * top, bound, skew, False)
    places = jnp.arange(number_of)

    def named(lengths, offset_by):
        used = int((lengths > 0).sum())
        fixed = max(1, used // 4)
        moved = fixed + (places - fixed + offset_by * (used - fixed)) % max(1, number_of - fixed)
        return jnp.zeros((number_of,), jnp.int32).at[order[jnp.where(places < fixed, places, moved)]].set(jnp.asarray(lengths, jnp.int32))

    lengths = jnp.where(number % 4 == 0, named(heavy_load, number // 4), named(common, number - number // 4 - 1))
    mixed = jax.random.permutation(jax.random.fold_in(own, 3), number_of)
    source_of, sink = mixed[0:number_of // 2 * 2:2], mixed[1:number_of // 2 * 2:2]
    room = jnp.minimum(lengths[source_of] - 1, bound - lengths[sink]) // 2
    room = jnp.where((source_of == order[0]) | (sink == order[0]) | (lengths[sink] == 0), 0, jnp.maximum(room, 0))
    moved = jax.random.randint(jax.random.fold_in(own, 4), (number_of // 2,), 0, 1 << 20) % (room + 1)
    lengths = lengths.at[source_of].add(-moved).at[sink].add(moved)
    members = jnp.searchsorted(jnp.cumsum(lengths), jnp.arange(rows * top), side="right").astype(jnp.int32)
    table = members.reshape(top, rows).T
    table = table[jax.random.permutation(jax.random.fold_in(own, 1), rows)]
    offset_by = jax.random.randint(jax.random.fold_in(own, 2), (rows, 1), 0, top)
    return jnp.take_along_axis(table, (jnp.arange(top)[None, :] + offset_by) % top, axis=1)


def load_shares(number_of, total, most, lean, full):
    weights = [(1 << 20) // math.isqrt(rank ** lean) + 1 for rank in range(1, number_of + 1)]
    largest = most if full else min(most, max(-(-total // number_of), total * weights[0] // sum(weights)))
    least = 1 if total - largest >= number_of - 1 else 0
    holding, spare = [largest] + [least] * (number_of - 1), total - largest - least * (number_of - 1)
    while spare > 0:
        free = [i for i in range(1, number_of) if holding[i] < largest] or [i for i in range(1, number_of) if holding[i] < most]
        whole, left = sum([weights[i] for i in free]), spare
        for i in free:
            addition = min(most - holding[i], max(1, left * weights[i] // whole), spare)
            holding[i] = holding[i] + addition
            spare = spare - addition
    return np.array(holding)


def scatter_about(rng, shape, scale, bound, cuts=(), kind=jnp.bfloat16):
    entries = scale * jax.random.normal(rng, shape, jnp.float32)
    if cuts:
        entries = entries * level_of(rng, shape, cuts, -0.22, 0.18)
    return jnp.clip(entries, -bound, bound).astype(kind)


def setup_inputs(seed: int = 0) -> dict:
    splits = jax.random.split(jax.random.key(seed), 20)
    skip_stream_entry = scatter_about(splits[0], (SERIES_ITEMS, WIDTH), 1.0, 6.0, ((0, 32),))
    result_switch_mapped = scatter_about(splits[1], (SERIES_ITEMS, INNER), 1.0, 6.0, ((0, 4), (1, 8)))
    channel_feed_mapped = scatter_about(splits[2], (SERIES_ITEMS, INNER), 1.0, 6.0, ((0, 4), (1, 8)))
    write_coefficient_mapped = scatter_about(splits[3], (SERIES_ITEMS, GROUPS * STATE), 1.0, 6.0, ((0, 4), (1, 8)))
    emission_coefficient_mapped = scatter_about(splits[4], (SERIES_ITEMS, GROUPS * STATE), 1.0, 6.0, ((0, 4), (1, 8)))
    channel_feed_taps = scatter_about(splits[5], (CONV_W, INNER), CONV_W ** -0.5, 2.5, ((1, 8),))
    write_coefficient_taps = scatter_about(splits[6], (CONV_W, GROUPS * STATE), CONV_W ** -0.5, 2.5, ((1, 8),))
    emission_coefficient_taps = scatter_about(splits[7], (CONV_W, GROUPS * STATE), CONV_W ** -0.5, 2.5, ((1, 8),))
    raw_increments = draw_raw_increments(jax.random.fold_in(splits[19], 71), 0)
    channel_log_fade_speed = draw_channel_log_fade_speed(jax.random.fold_in(splits[19], 71), 0)
    extra_log_fade = draw_extra_log_fade(jax.random.fold_in(splits[19], 71), 0)
    cluster_scaling_factor = jnp.clip(1.0 + 0.18 * jax.random.normal(splits[11], (INNER,), jnp.float32), 0.1, 1.9)
    blend_result_matrix = scatter_about(splits[12], (INNER, WIDTH), INNER ** -0.5, 0.09375, ((0, 8),))
    routing_scaling_factor = jnp.clip(1.0 + 0.18 * jax.random.normal(splits[13], (WIDTH,), jnp.float32), 0.1, 1.9)
    specialist_switch_matrix = scatter_about(splits[14], (EXPERTS, WIDTH, EXPERT_FF), WIDTH ** -0.5, 0.125, ((0, 4), (2, 8)))
    specialist_widen_matrix = scatter_about(splits[15], (EXPERTS, WIDTH, EXPERT_FF), WIDTH ** -0.5, 0.125, ((0, 4), (2, 8)))
    specialist_contract_matrix = scatter_about(splits[16], (EXPERTS, EXPERT_FF, WIDTH), (EXPERT_FF // 4) ** -0.5, 0.1875, ((0, 4), (1, 8)))
    picked_specialists_keys = jax.random.split(jax.random.fold_in(splits[17], 1), SERIES_ITEMS // ROWS_DEV)
    picked_specialists_turns = jax.random.permutation(jax.random.fold_in(splits[17], 3), SERIES_ITEMS // ROWS_DEV)
    picked_specialists = jax.vmap(lambda own, number: shared_out(jax.random.fold_in(splits[17], 2), own, number, ROWS_DEV, EXPERTS, TOP, CAPACITY, 1))(picked_specialists_keys, picked_specialists_turns).reshape((SERIES_ITEMS, TOP))
    router_affinities = jnp.clip(jnp.exp(math.log(1.0) - 2.3025851 * jax.random.uniform(splits[18], (SERIES_ITEMS, TOP), jnp.float32) ** level_of(splits[18], (SERIES_ITEMS, TOP), ((0, 32),), -0.2, 0.2)), 0.1, 1.0)
    return dict(skip_stream_entry=skip_stream_entry, result_switch_mapped=result_switch_mapped, channel_feed_mapped=channel_feed_mapped, write_coefficient_mapped=write_coefficient_mapped, emission_coefficient_mapped=emission_coefficient_mapped, channel_feed_taps=channel_feed_taps, write_coefficient_taps=write_coefficient_taps, emission_coefficient_taps=emission_coefficient_taps, raw_increments=raw_increments, channel_log_fade_speed=channel_log_fade_speed, extra_log_fade=extra_log_fade, cluster_scaling_factor=cluster_scaling_factor, blend_result_matrix=blend_result_matrix, routing_scaling_factor=routing_scaling_factor, specialist_switch_matrix=specialist_switch_matrix, specialist_widen_matrix=specialist_widen_matrix, specialist_contract_matrix=specialist_contract_matrix, picked_specialists=picked_specialists, router_affinities=router_affinities)


EPSILON = 1e-06
HIGHEST_MODE = lax.Precision.HIGHEST

def centred_conv(padded, weights, series_count):
    summed = jnp.zeros((series_count, padded.shape[1]), jnp.float32)
    for offset in range(weights.shape[0]):
        summed = summed + weights[offset].astype(jnp.float32) * padded[offset:offset + series_count].astype(jnp.float32)
    return jax.nn.silu(summed)

def local_sweep(inputs, entry_state, readout_state, log_fade_factor, softplus_increment):
    seq_len = inputs.shape[0]
    blocks = seq_len // BLOCK
    heads_here = log_fade_factor.shape[0]
    groups_here = entry_state.shape[1] // STATE
    per_group = heads_here // groups_here
    values = inputs.reshape(blocks, BLOCK, groups_here, per_group, HEAD_DIM)
    b_blocks = entry_state.reshape(blocks, BLOCK, groups_here, STATE)
    c_blocks = readout_state.reshape(blocks, BLOCK, groups_here, STATE)
    decay_blocks = log_fade_factor.reshape(groups_here, per_group, blocks, BLOCK)
    step_blocks = softplus_increment.reshape(groups_here, per_group, blocks, BLOCK)
    cumulative = jnp.cumsum(decay_blocks, axis=-1)
    group_inner = jnp.einsum('bign,bjgn->gbij', c_blocks, b_blocks, precision=HIGHEST_MODE)
    spread = cumulative[..., :, None] - cumulative[..., None, :]
    lower_tri = jnp.arange(BLOCK)[:, None] >= jnp.arange(BLOCK)[None, :]
    mixing = jnp.exp(jnp.where(lower_tri, spread, -jnp.inf)) * step_blocks[..., None, :] * group_inner[:, None]
    within = jnp.einsum('gkbij,bjgkp->bigkp', mixing, values, precision=HIGHEST_MODE)
    to_end = jnp.exp(cumulative[..., -1:] - cumulative) * step_blocks
    block_states = jnp.einsum('gkbj,bjgkp,bjgn->bgkpn', to_end, values, b_blocks, precision=HIGHEST_MODE)
    block_decay = cumulative[..., -1]

    def advance(carried, pieces):
        state_piece, decay_piece = pieces
        return (carried * jnp.exp(decay_piece)[..., None, None] + state_piece, carried)
    zero_state = jnp.zeros((groups_here, per_group, HEAD_DIM, STATE), jnp.float32)
    final_state, entering = lax.scan(advance, zero_state, (block_states, jnp.moveaxis(block_decay, -1, 0)))
    before = jnp.cumsum(block_decay, axis=-1) - block_decay
    return ((within, entering, cumulative, before, c_blocks), (lax.optimization_barrier(jnp.sum(block_decay, axis=-1)), final_state))

def finish_sweep(parts, carried):
    within, entering, cumulative, before, c_blocks = parts
    entering = entering + carried[None] * jnp.exp(jnp.moveaxis(before, -1, 0))[..., None, None]
    readout = jnp.einsum('bign,bgkpn->bigkp', c_blocks, entering, precision=HIGHEST_MODE)
    readout = readout * jnp.exp(jnp.transpose(cumulative, (2, 3, 0, 1)))[..., None]
    combined = within + readout
    return combined.reshape(combined.shape[0] * combined.shape[1], -1)

def blend_parts_list(channel_feed_bordered, write_coefficient_bordered, emission_coefficient_bordered, channel_feed_taps, write_coefficient_taps, emission_coefficient_taps, raw_increments, channel_log_fade_speed, extra_log_fade, series_count):
    inputs = centred_conv(channel_feed_bordered, channel_feed_taps, series_count)
    entry_state = centred_conv(write_coefficient_bordered, write_coefficient_taps, series_count)
    readout_state = centred_conv(emission_coefficient_bordered, emission_coefficient_taps, series_count)
    softplus_increment = jax.nn.softplus(raw_increments.astype(jnp.float32))
    log_fade_factor = -softplus_increment * jnp.exp(channel_log_fade_speed)[..., None] + extra_log_fade
    onward_pass = local_sweep(inputs, entry_state, readout_state, log_fade_factor[0], softplus_increment[0])
    backward_pass = local_sweep(jnp.flip(inputs, 0), jnp.flip(entry_state, 0), jnp.flip(readout_state, 0), jnp.flip(log_fade_factor[1], -1), jnp.flip(softplus_increment[1], -1))
    return (onward_pass, backward_pass)

def gated_norm(mixed_sum, result_switch_mapped, cluster_scaling_factor):
    gated = mixed_sum * jax.nn.silu(result_switch_mapped.astype(jnp.float32))
    grouped = gated.reshape(gated.shape[0], -1, INNER // GROUPS)
    normalized = grouped * lax.rsqrt(lax.optimization_barrier(jnp.mean(grouped * grouped, axis=-1, keepdims=True)) + EPSILON)
    return (normalized.reshape(gated.shape) * cluster_scaling_factor).astype(jnp.bfloat16)

def rms_scale(stream, gain):
    values = stream.astype(jnp.float32)
    return (values * lax.rsqrt(lax.optimization_barrier(jnp.mean(values * values, axis=-1, keepdims=True)) + EPSILON) * gain).astype(jnp.bfloat16)

def reference(skip_stream_entry, result_switch_mapped, channel_feed_mapped, write_coefficient_mapped, emission_coefficient_mapped, channel_feed_taps, write_coefficient_taps, emission_coefficient_taps, raw_increments, channel_log_fade_speed, extra_log_fade, cluster_scaling_factor, blend_result_matrix, routing_scaling_factor, specialist_switch_matrix, specialist_widen_matrix, specialist_contract_matrix, picked_specialists, router_affinities):
    rim_width = CONV_W // 2
    filter_border_width = ((rim_width, rim_width), (0, 0))
    onward_pass, backward_pass = blend_parts_list(jnp.pad(channel_feed_mapped, filter_border_width), jnp.pad(write_coefficient_mapped, filter_border_width), jnp.pad(emission_coefficient_mapped, filter_border_width), channel_feed_taps, write_coefficient_taps, emission_coefficient_taps, raw_increments, channel_log_fade_speed, extra_log_fade, SERIES_ITEMS)
    zero_carry = jnp.zeros_like(onward_pass[1][1])
    mixed_sum = finish_sweep(onward_pass[0], zero_carry) + jnp.flip(finish_sweep(backward_pass[0], zero_carry), 0)
    mixed_rows = gated_norm(mixed_sum, result_switch_mapped, cluster_scaling_factor)
    slice_width = INNER // N_TP

    def add_slice(summed, slice_index):
        columns = lax.dynamic_slice_in_dim(mixed_rows, slice_index * slice_width, slice_width, 1)
        weights = lax.dynamic_slice_in_dim(blend_result_matrix, slice_index * slice_width, slice_width, 0)
        partial_sum = jnp.dot(columns, weights, preferred_element_type=jnp.float32).astype(jnp.bfloat16)
        partial_sum = lax.optimization_barrier(partial_sum)
        return (summed + partial_sum.astype(jnp.float32), slice_index)
    projected = lax.scan(add_slice, jnp.zeros((SERIES_ITEMS, WIDTH), jnp.float32), jnp.arange(N_TP, dtype=jnp.int32))[0]
    after_mixer = (skip_stream_entry.astype(jnp.float32) + projected).astype(jnp.bfloat16)
    normed = rms_scale(after_mixer, routing_scaling_factor)
    row_count = SERIES_ITEMS * TOP
    flat_routes = picked_specialists.reshape(row_count)
    owner = jnp.arange(row_count, dtype=jnp.int32) // TOP
    limit = N_SP * N_TP * CAPACITY
    ff_slice = EXPERT_FF // N_TP

    def one_expert(outputs, expert):
        chosen = flat_routes == expert
        chosen_rank = jnp.cumsum(chosen.astype(jnp.int32)) - 1
        target = jnp.where(chosen, chosen_rank, limit)
        member = jnp.zeros((limit,), jnp.int32).at[target].set(jnp.arange(row_count, dtype=jnp.int32), mode='drop')
        filled = jnp.zeros((limit,), jnp.int32).at[target].set(1, mode='drop')
        picked = normed[owner[member]]
        gate_part = jnp.dot(picked, specialist_switch_matrix[expert], preferred_element_type=jnp.float32)
        up_part = jnp.dot(picked, specialist_widen_matrix[expert], preferred_element_type=jnp.float32)
        hidden = (jax.nn.silu(gate_part) * up_part).astype(jnp.bfloat16)
        pieces = jnp.einsum('rsf,sfd->rsd', hidden.reshape(limit, N_TP, ff_slice).astype(jnp.float32), specialist_contract_matrix[expert].reshape(N_TP, ff_slice, WIDTH).astype(jnp.float32))
        pieces = lax.optimization_barrier(pieces.astype(jnp.bfloat16))
        expert_out = lax.optimization_barrier(jnp.sum(pieces.astype(jnp.float32), axis=1)).astype(jnp.bfloat16)
        destination = jnp.where(filled > 0, member, row_count)
        return (outputs.at[destination].set(expert_out, mode='drop'), expert)
    assigned = lax.scan(one_expert, jnp.zeros((row_count, WIDTH), jnp.bfloat16), jnp.arange(EXPERTS, dtype=jnp.int32))[0]
    weights = router_affinities / lax.optimization_barrier(jnp.sum(router_affinities, axis=-1, keepdims=True))
    mixture = lax.optimization_barrier(jnp.sum(weights[..., None] * assigned.reshape(SERIES_ITEMS, TOP, WIDTH).astype(jnp.float32), axis=1))
    return (after_mixer.astype(jnp.float32) + mixture).astype(jnp.bfloat16)
```

```python
import functools

import jax
import jax.numpy as jnp
from jax import lax
from jax.experimental import pallas as pl
from jax.experimental.pallas import tpu as pltpu
from jax.sharding import PartitionSpec as P

WIDTH = 2048
HEAD_DIM = 64
GROUPS = 16
STATE = 128
CONV_W = 5
BLOCK = 128
TOP = 2
INNER = 4096


EPSILON = 1e-06
HIGHEST_MODE = lax.Precision.HIGHEST


MESH_IDS = pl.DeviceIdType.MESH


def neighbour_rows(rows, axis, step):
    count = lax.axis_size(axis)
    pairs = [(i, i + step) for i in range(count) if 0 <= i + step < count]
    return lax.ppermute(rows, axis, pairs)


def spread_heads(columns, per_group):
    rows = columns.shape[0]
    lane = lax.broadcasted_iota(jnp.int32, (rows, per_group * HEAD_DIM), 1) // HEAD_DIM
    out = jnp.broadcast_to(columns[:, 0:1], lane.shape)
    for head in range(1, per_group):
        out = jnp.where(lane == head, jnp.broadcast_to(columns[:, head : head + 1], lane.shape), out)
    return out


def silu(value):
    return value * jax.nn.sigmoid(value)


def fill_padded(scratch, source, low, high):
    count, rim = source.shape[0], low.shape[0]
    scratch[8 : 8 + count, :] = source[...].astype(jnp.float32)
    scratch[8 - rim : 8, :] = low[...].astype(jnp.float32)
    scratch[8 + count : 8 + count + rim, :] = high[...].astype(jnp.float32)


def conv_block(scratch, taps, block):
    rim = taps.shape[0] // 2
    total = None
    for offset in range(taps.shape[0]):
        start = 8 - rim + offset + block * BLOCK
        term = taps[offset : offset + 1, :].astype(jnp.float32) * scratch[start : start + BLOCK, :]
        total = term if total is None else total + term
    return silu(total)


def sweep_kernel(
    x_ref, b_ref, c_ref, x_low, x_high, b_low, b_high, c_low, c_high, x_taps, b_taps, c_taps,
    fade_ref, y_ref, c_out, state_ref, reach_ref, x_pad, b_pad, c_pad, entry_scr,
):
    count, width = x_ref.shape
    blocks = count // BLOCK
    per_group = width // HEAD_DIM
    rows = 2 * per_group
    fill_padded(x_pad, x_ref, x_low, x_high)
    fill_padded(b_pad, b_ref, b_low, b_high)
    fill_padded(c_pad, c_ref, c_low, c_high)
    i_at = lax.broadcasted_iota(jnp.int32, (BLOCK, BLOCK), 0)
    j_at = lax.broadcasted_iota(jnp.int32, (BLOCK, BLOCK), 1)
    up_to = (i_at <= j_at).astype(jnp.float32)
    from_on = (i_at >= j_at).astype(jnp.float32)
    row_at = lax.broadcasted_iota(jnp.int32, (rows, BLOCK), 0)
    col_at = lax.broadcasted_iota(jnp.int32, (1, rows), 1)
    half_lane = lax.broadcasted_iota(jnp.int32, (BLOCK, 2 * HEAD_DIM), 1) < HEAD_DIM
    totals, parts, columns_kept, mixed = [], [], [], []
    for block in range(blocks):
        at = slice(block * BLOCK, (block + 1) * BLOCK)
        fade = fade_ref[0, 0:rows, at]
        step = fade_ref[0, rows : 2 * rows, at]
        onward = jnp.dot(fade, up_to, precision=HIGHEST_MODE, preferred_element_type=jnp.float32)
        back = jnp.dot(fade, from_on, precision=HIGHEST_MODE, preferred_element_type=jnp.float32)
        cum = jnp.where(row_at < per_group, onward, back)
        stacked = jnp.concatenate(
            [cum, step, jnp.zeros((BLOCK - 2 * rows, BLOCK), jnp.float32)], axis=0
        )
        turned = jnp.transpose(stacked)
        cum_col, step_col = turned[:, 0:rows], turned[:, rows : 2 * rows]
        total = jnp.where(col_at < per_group, cum_col[BLOCK - 1 : BLOCK, :], cum_col[0:1, :])
        to_end = jnp.exp(total - cum_col) * step_col
        x = conv_block(x_pad, x_taps, block)
        b = conv_block(b_pad, b_taps, block)
        c = conv_block(c_pad, c_taps, block).astype(jnp.bfloat16)
        c_out[at, :] = c
        b_turned = jnp.transpose(b).astype(jnp.bfloat16)
        weighted = jnp.concatenate(
            [
                x * spread_heads(to_end[:, 0:per_group], per_group),
                x * spread_heads(to_end[:, per_group:rows], per_group),
            ],
            axis=1,
        ).astype(jnp.bfloat16)
        parts.append(jnp.dot(b_turned, weighted, preferred_element_type=jnp.float32))
        inner = jnp.dot(c, b_turned, preferred_element_type=jnp.float32)
        mixing = []
        for head in range(per_group):
            other = per_group + head
            gap = jnp.where(
                i_at >= j_at,
                cum_col[:, head : head + 1] - cum[head : head + 1, :],
                cum_col[:, other : other + 1] - cum[other : other + 1, :],
            )
            own, opposite = step[head : head + 1, :], step[other : other + 1, :]
            amount = jnp.where(
                i_at > j_at, own, jnp.where(i_at < j_at, opposite, own + opposite)
            )
            mixing.append((jnp.exp(gap) * amount * inner).astype(jnp.bfloat16))
        pieces = []
        for pair in range(per_group // 2):
            x_pair = x[:, pair * 2 * HEAD_DIM : (pair + 1) * 2 * HEAD_DIM]
            both = jnp.concatenate(
                [jnp.where(half_lane, x_pair, 0.0), jnp.where(half_lane, 0.0, x_pair)], axis=0
            ).astype(jnp.bfloat16)
            left = jnp.concatenate([mixing[2 * pair], mixing[2 * pair + 1]], axis=1)
            pieces.append(jnp.dot(left, both, preferred_element_type=jnp.float32))
        y_ref[at, :] = jnp.concatenate(pieces, axis=1)
        totals.append(total)
        columns_kept.append(cum_col)
    for first, order in ((0, range(blocks)), (1, range(blocks - 1, -1, -1))):
        lanes = slice(first * width, (first + 1) * width)
        held = jnp.zeros((STATE, width), jnp.float32)
        for block in order:
            entry_scr[block, :, lanes] = held.astype(jnp.bfloat16)
            factor = spread_heads(
                jnp.exp(totals[block][:, first * per_group : (first + 1) * per_group]), per_group
            )
            held = held * factor + parts[block][:, lanes]
        state_ref[first, 0, 0:STATE, :] = held.astype(jnp.bfloat16)
        whole = totals[0]
        for block in range(1, blocks):
            whole = whole + totals[block]
        whole = spread_heads(
            jnp.exp(whole[:, first * per_group : (first + 1) * per_group]), per_group
        )
        state_ref[first, 0, STATE:, :] = jnp.broadcast_to(
            whole, (state_ref.shape[2] - STATE, width)
        ).astype(jnp.bfloat16)
    for block in range(blocks):
        at = slice(block * BLOCK, (block + 1) * BLOCK)
        readout = jnp.dot(c_out[at, :], entry_scr[block], preferred_element_type=jnp.float32)
        fade_in = jnp.exp(columns_kept[block])
        y_ref[at, :] = (
            y_ref[at, :]
            + readout[:, :width] * spread_heads(fade_in[:, 0:per_group], per_group)
            + readout[:, width:] * spread_heads(fade_in[:, per_group:rows], per_group)
        )
        offset = jnp.zeros((1, rows), jnp.float32)
        for earlier in range(blocks):
            if earlier < block:
                offset = offset + jnp.where(col_at < per_group, totals[earlier], 0.0)
            if earlier > block:
                offset = offset + jnp.where(col_at < per_group, 0.0, totals[earlier])
        reach_ref[0, at, :] = jnp.exp(columns_kept[block] + offset)


def exchange_kernel(axis, source, target, send_sem, recv_sem):
    here, peers = lax.axis_index(axis), lax.axis_size(axis)
    barrier = pltpu.get_barrier_semaphore()
    for away in range(1, peers):
        pl.semaphore_signal(
            barrier, inc=1, device_id={axis: lax.rem(here + away, peers)}, device_id_type=MESH_IDS
        )
    pl.semaphore_wait(barrier, peers - 1)
    copies = []
    for away in range(1, peers):
        peer = lax.rem(here + away, peers)
        copies.append(
            pltpu.make_async_remote_copy(
                src_ref=source.at[jnp.where(peer > here, 0, 1)],
                dst_ref=target.at[here],
                send_sem=send_sem.at[away - 1],
                recv_sem=recv_sem.at[away - 1],
                device_id={axis: peer},
                device_id_type=MESH_IDS,
            )
        )
    for copy in copies:
        copy.start()
    target[here] = jnp.zeros(target.shape[1:], target.dtype)
    for copy in copies:
        copy.wait()


def blend_kernel(
    here_ref, y_ref, c_ref, reach_ref, states_ref, gate_ref, gain_ref, weight_ref, out_ref, carry_scr
):
    peers, groups, _, width = states_ref.shape
    per_group = width // HEAD_DIM
    rows = 2 * per_group

    @pl.when(pl.program_id(0) == 0)
    def _():
        here = here_ref[0]
        for group in range(groups):
            for first in range(2):
                held = jnp.zeros((STATE, width), jnp.float32)
                order = range(peers) if first == 0 else range(peers - 1, -1, -1)
                for peer in order:
                    fresh = states_ref[peer, group, 0:STATE, :].astype(jnp.float32)
                    factor = states_ref[peer, group, STATE : STATE + 1, :].astype(jnp.float32)
                    reached = peer < here if first == 0 else peer > here
                    held = jnp.where(reached, held * factor + fresh, held)
                carry_scr[group, :, first * width : (first + 1) * width] = held.astype(jnp.bfloat16)

    mixed = []
    for group in range(groups):
        lanes = slice(group * width, (group + 1) * width)
        c = c_ref[:, group * STATE : (group + 1) * STATE]
        readout = jnp.dot(c, carry_scr[group], preferred_element_type=jnp.float32)
        reach = reach_ref[group]
        y = (
            y_ref[:, lanes]
            + readout[:, :width] * spread_heads(reach[:, 0:per_group], per_group)
            + readout[:, width:] * spread_heads(reach[:, per_group:rows], per_group)
        )
        gated = y * silu(gate_ref[:, lanes].astype(jnp.float32))
        square = jnp.mean(gated * gated, axis=-1, keepdims=True)
        mixed.append((gated * lax.rsqrt(square + EPSILON) * gain_ref[:, lanes]).astype(jnp.bfloat16))
    rows_mixed = mixed[0] if groups == 1 else jnp.concatenate(mixed, axis=1)
    out_ref[...] = jnp.dot(
        rows_mixed, weight_ref[...], preferred_element_type=jnp.float32
    ).astype(jnp.bfloat16)


def mixer(
    result_switch_mapped, channel_feed_mapped, write_coefficient_mapped,
    emission_coefficient_mapped, channel_feed_taps, write_coefficient_taps,
    emission_coefficient_taps, raw_increments, channel_log_fade_speed, extra_log_fade,
    cluster_scaling_factor, blend_result_matrix,
):
    count, inner_here = channel_feed_mapped.shape
    groups = write_coefficient_mapped.shape[1] // STATE
    width = inner_here // groups
    per_group = width // HEAD_DIM
    rim = channel_feed_taps.shape[0] // 2
    sources = (channel_feed_mapped, write_coefficient_mapped, emission_coefficient_mapped)
    low = neighbour_rows(jnp.concatenate([s[-rim:] for s in sources], 1), "sp", 1)
    high = neighbour_rows(jnp.concatenate([s[:rim] for s in sources], 1), "sp", -1)
    cuts = (inner_here, inner_here + groups * STATE)
    lows, highs = jnp.split(low, cuts, axis=1), jnp.split(high, cuts, axis=1)
    step = jax.nn.softplus(raw_increments.astype(jnp.float32))
    fade = -step * jnp.exp(channel_log_fade_speed)[..., None] + extra_log_fade

    def by_group(value):
        value = value.reshape(2, groups, per_group, count)
        return jnp.transpose(value, (1, 0, 2, 3)).reshape(groups, 2 * per_group, count)

    fades = jnp.concatenate([by_group(fade), by_group(step)], axis=1)
    rows = 2 * per_group
    depth = STATE + 16

    def wide(height):
        return pl.BlockSpec((height, width), lambda g: (0, g))

    def narrow(height):
        return pl.BlockSpec((height, STATE), lambda g: (0, g))

    taps = channel_feed_taps.shape[0]
    y, c, states, reach = pl.pallas_call(
        sweep_kernel,
        grid=(groups,),
        in_specs=[
            wide(count), narrow(count), narrow(count), wide(rim), wide(rim), narrow(rim),
            narrow(rim), narrow(rim), narrow(rim), wide(taps), narrow(taps), narrow(taps),
            pl.BlockSpec((1, 2 * rows, count), lambda g: (g, 0, 0)),
        ],
        out_specs=[
            wide(count), narrow(count),
            pl.BlockSpec((2, 1, depth, width), lambda g: (0, g, 0, 0)),
            pl.BlockSpec((1, count, rows), lambda g: (g, 0, 0)),
        ],
        out_shape=[
            jax.ShapeDtypeStruct((count, inner_here), jnp.float32),
            jax.ShapeDtypeStruct((count, groups * STATE), jnp.bfloat16),
            jax.ShapeDtypeStruct((2, groups, depth, width), jnp.bfloat16),
            jax.ShapeDtypeStruct((groups, count, rows), jnp.float32),
        ],
        scratch_shapes=[
            pltpu.VMEM((count + 16, width), jnp.float32),
            pltpu.VMEM((count + 16, STATE), jnp.float32),
            pltpu.VMEM((count + 16, STATE), jnp.float32),
            pltpu.VMEM((count // BLOCK, STATE, 2 * width), jnp.bfloat16),
        ],
        cost_estimate=pl.CostEstimate(flops=200_000_000, bytes_accessed=4_000_000, transcendentals=0),
        name="sweep",
    )(
        *sources, lows[0], highs[0], lows[1], highs[1], lows[2], highs[2],
        channel_feed_taps, write_coefficient_taps, emission_coefficient_taps, fades,
    )
    peers = lax.axis_size("sp")
    gathered = pl.pallas_call(
        functools.partial(exchange_kernel, "sp"),
        in_specs=[pl.BlockSpec(memory_space=pltpu.VMEM)],
        out_specs=pl.BlockSpec(memory_space=pltpu.VMEM),
        out_shape=jax.ShapeDtypeStruct((peers,) + states.shape[1:], jnp.bfloat16),
        scratch_shapes=[
            pltpu.SemaphoreType.DMA((peers - 1,)),
            pltpu.SemaphoreType.DMA((peers - 1,)),
        ],
        compiler_params=pltpu.CompilerParams(collective_id=0, has_side_effects=True),
        name="exchange",
    )(states)
    features = blend_result_matrix.shape[1]
    here = jnp.full((1,), lax.axis_index("sp"), jnp.int32)
    return pl.pallas_call(
        blend_kernel,
        grid=(count // BLOCK,),
        in_specs=[
            pl.BlockSpec(memory_space=pltpu.SMEM),
            pl.BlockSpec((BLOCK, inner_here), lambda i: (i, 0)),
            pl.BlockSpec((BLOCK, groups * STATE), lambda i: (i, 0)),
            pl.BlockSpec((groups, BLOCK, rows), lambda i: (0, i, 0)),
            pl.BlockSpec(gathered.shape, lambda i: (0, 0, 0, 0)),
            pl.BlockSpec((BLOCK, inner_here), lambda i: (i, 0)),
            pl.BlockSpec((1, inner_here), lambda i: (0, 0)),
            pl.BlockSpec(blend_result_matrix.shape, lambda i: (0, 0)),
        ],
        out_specs=pl.BlockSpec((BLOCK, features), lambda i: (i, 0)),
        out_shape=jax.ShapeDtypeStruct((count, features), jnp.bfloat16),
        scratch_shapes=[pltpu.VMEM((groups, STATE, 2 * width), jnp.bfloat16)],
        name="blend",
    )(
        here, y, c, reach, gathered, result_switch_mapped,
        cluster_scaling_factor.reshape(1, -1), blend_result_matrix,
    )


def rms_scale(stream, gain):
    values = stream.astype(jnp.float32)
    return (
        values * lax.rsqrt(jnp.mean(values * values, axis=-1, keepdims=True) + EPSILON) * gain
    ).astype(jnp.bfloat16)


def per_device(
    skip_stream_entry,
    result_switch_mapped,
    channel_feed_mapped,
    write_coefficient_mapped,
    emission_coefficient_mapped,
    channel_feed_taps,
    write_coefficient_taps,
    emission_coefficient_taps,
    raw_increments,
    channel_log_fade_speed,
    extra_log_fade,
    cluster_scaling_factor,
    blend_result_matrix,
    routing_scaling_factor,
    specialist_switch_matrix,
    specialist_widen_matrix,
    specialist_contract_matrix,
    picked_specialists,
    router_affinities,
):
    partial = mixer(
        result_switch_mapped, channel_feed_mapped, write_coefficient_mapped,
        emission_coefficient_mapped, channel_feed_taps, write_coefficient_taps,
        emission_coefficient_taps, raw_increments, channel_log_fade_speed, extra_log_fade,
        cluster_scaling_factor, blend_result_matrix,
    )
    rows_here = skip_stream_entry.shape[0]
    projected = lax.psum_scatter(
        partial,
        "tp",
        scatter_dimension=0,
        tiled=True,
    ).astype(jnp.float32)
    after_mixer = (skip_stream_entry.astype(jnp.float32) + projected).astype(jnp.bfloat16)
    normed = rms_scale(after_mixer, routing_scaling_factor)
    experts_here = specialist_switch_matrix.shape[0]
    expert_count = experts_here * lax.axis_size("sp")
    capacity = max(2, 3 * TOP * rows_here // (2 * expert_count))
    peers = lax.axis_size("sp")
    slot_total = capacity * peers
    flat_routes = picked_specialists.reshape(-1)
    one_hot = (flat_routes[:, None] == jnp.arange(expert_count, dtype=jnp.int32)[None, :]).astype(
        jnp.int32
    )
    earlier_count = jnp.cumsum(one_hot, axis=0) - one_hot
    slot_rank = jnp.sum(earlier_count * one_hot, axis=1)
    position = (flat_routes // experts_here) * capacity + slot_rank
    matches, blocks = [], []
    for expert in range(experts_here):
        place = jnp.where(flat_routes % experts_here == expert, position, -1)
        match = (place[:, None] == jnp.arange(slot_total, dtype=jnp.int32)[None, :]).astype(
            jnp.bfloat16
        )
        token_match = jnp.sum(match.reshape(rows_here, TOP, slot_total), axis=1)
        buffer = jnp.einsum(
            "rs,rd->sd", token_match, normed, preferred_element_type=jnp.float32
        ).astype(jnp.bfloat16)
        received = lax.all_to_all(buffer, "sp", split_axis=0, concat_axis=0, tiled=True)
        matches.append(match)
        blocks.append(lax.all_gather(received, "tp", axis=0, tiled=True))
    picked = jnp.zeros((rows_here * TOP, WIDTH), jnp.float32)
    for expert in range(experts_here):
        gate_part = jnp.dot(
            blocks[expert], specialist_switch_matrix[expert], preferred_element_type=jnp.float32
        )
        up_part = jnp.dot(
            blocks[expert], specialist_widen_matrix[expert], preferred_element_type=jnp.float32
        )
        hidden = (jax.nn.silu(gate_part) * up_part).astype(jnp.bfloat16)
        expert_out = lax.psum_scatter(
            jnp.dot(
                hidden, specialist_contract_matrix[expert], preferred_element_type=jnp.float32
            ).astype(jnp.bfloat16),
            "tp",
            scatter_dimension=0,
            tiled=True,
        )
        returned = lax.all_to_all(expert_out, "sp", split_axis=0, concat_axis=0, tiled=True)
        picked = picked + jnp.dot(matches[expert], returned, preferred_element_type=jnp.float32)
    weights = router_affinities / jnp.sum(router_affinities, axis=-1, keepdims=True)
    mixture = jnp.sum(weights[..., None] * picked.reshape(rows_here, TOP, WIDTH), axis=1)
    return (after_mixer.astype(jnp.float32) + mixture).astype(jnp.bfloat16)


def solution(mesh):
    in_specs = (
        P(("sp", "tp"), None),
        P("sp", "tp"),
        P("sp", "tp"),
        P("sp", "tp"),
        P("sp", "tp"),
        P(None, "tp"),
        P(None, "tp"),
        P(None, "tp"),
        P(None, "tp", "sp"),
        P(None, "tp"),
        P(None, "tp", "sp"),
        P("tp"),
        P("tp", None),
        P(),
        P("sp", None, "tp"),
        P("sp", None, "tp"),
        P("sp", "tp", None),
        P(("sp", "tp"), None),
        P(("sp", "tp"), None),
    )
    out_specs = P(("sp", "tp"), None)
    return jax.shard_map(
        per_device, mesh=mesh, in_specs=in_specs, out_specs=out_specs, check_vma=False
    )
```
